32 devices in a mesh: fs: 16 (over z, y, x), tp: 2 (over core).
Axes of the slice: x: 2, y: 2, z: 4, core: 2. Of those that a mesh axis runs over, the one named last changes fastest.
Arguments:
- block_input: bfloat16 [16384, 2048], P('fs'), may hold values from -6 to 6
- value_cotangent: bfloat16 [16384, 1024], P('fs', 'tp'), may hold values from -6 to 6
- mixed_output: bfloat16 [16384, 1024], P('fs', 'tp'), may hold values from -6 to 6
- output_cotangent: bfloat16 [16384, 2048], P('fs'), may hold values from -6 to 6
- value_weight: float32 [2048, 1024], P('fs', 'tp'), may hold values from -0.125 to 0.125
- output_weight: float32 [1024, 2048], P('tp', 'fs'), may hold values from -0.1875 to 0.1875
- value_basis: bfloat16 [2048, 384], P('fs'), may hold values from -0.125 to 0.125
- output_basis: bfloat16 [2048, 384], P('fs'), may hold values from -0.125 to 0.125
- value_mean: float32 [384, 1024], P(None, 'tp'), may hold values from -4 to 4
- value_square: float32 [384, 1024], P(None, 'tp'), may hold values from 0.3 to 2
- output_mean: float32 [1024, 384], P('tp'), may hold values from -4 to 4
- output_square: float32 [1024, 384], P('tp'), may hold values from 0.3 to 2
Outputs:
- value_next: float32 [2048, 1024], P('fs', 'tp')
- value_copy: bfloat16 [2048, 1024], P(None, 'tp')
- value_step: float32 [2048, 1024], P('fs', 'tp')
- value_mean_next: float32 [384, 1024], P(None, 'tp')
- value_square_next: float32 [384, 1024], P(None, 'tp')
- output_next: float32 [1024, 2048], P('tp', 'fs')
- output_copy: bfloat16 [1024, 2048], P('tp')
- output_step: float32 [1024, 2048], P('tp', 'fs')
- output_mean_next: float32 [1024, 384], P('tp')
- output_square_next: float32 [1024, 384], P('tp')
The draws below stay inside these ranges and needn't reach their ends.
All inputs are finite; a program needn't handle non-finite values.
Results may differ from the reference program's by a relative error of at most 0.002.
Values may be sent and summed in bfloat16 or wider, within the bound.
No kernel may reach another device: no remote copies, remote signals or barrier semaphores. Data moves between devices by JAX's collectives and lax.ppermute only.
A program may use at most 64 MiB of HBM per device.

```python
import math
import jax
import jax.numpy as jnp
from jax import lax

D = 2048
E = 1024
R = 384
TOKENS = 16384


def block_scale(own_key, dims, shards, smallest, high):
    loudness = 1.0
    for axis_at, parts in shards:
        draws = jax.random.uniform(jax.random.fold_in(jax.random.fold_in(own_key, 6), axis_at), (parts,), jnp.float32, smallest / len(shards), high / len(shards))
        loudness = loudness * jnp.repeat(jnp.exp(draws), dims[axis_at] // parts).reshape((-1,) + (1,) * (len(dims) - 1 - axis_at))
    return loudness


def normal_values(own_key, dims, spread, limit, pieces=(), kind=jnp.bfloat16):
    drawn = spread * jax.random.normal(own_key, dims, jnp.float32)
    if pieces:
        drawn = drawn * block_scale(own_key, dims, pieces, -0.22, 0.18)
    return jnp.clip(drawn, -limit, limit).astype(kind)


def setup_inputs(seed: int = 0) -> dict:
    keys = jax.random.split(jax.random.key(seed), 13)
    return {
        "block_input": normal_values(keys[0], (TOKENS, D), 1.0, 6.0, ((0, 16),)),
        "value_cotangent": normal_values(keys[1], (TOKENS, E), 1.0, 6.0, ((0, 16), (1, 2))),
        "mixed_output": normal_values(keys[2], (TOKENS, E), 1.0, 6.0, ((0, 16), (1, 2))),
        "output_cotangent": normal_values(keys[3], (TOKENS, D), 1.0, 6.0, ((0, 16),)),
        "value_weight": normal_values(keys[4], (D, E), D ** -0.5, 0.125, ((0, 16), (1, 2)), jnp.float32),
        "output_weight": normal_values(keys[5], (E, D), E ** -0.5, 0.1875, ((0, 2), (1, 16)), jnp.float32),
        "value_basis": normal_values(keys[6], (D, R), D ** -0.5, 0.125, ((0, 16),)),
        "output_basis": normal_values(keys[7], (D, R), D ** -0.5, 0.125, ((0, 16),)),
        "value_mean": normal_values(keys[8], (R, E), 0.7, 4.0, ((1, 2),), jnp.float32),
        "value_square": jnp.clip(jnp.exp(math.log(2.0) - 1.89712 * jax.random.uniform(keys[9], (R, E), jnp.float32) ** block_scale(keys[9], (R, E), ((1, 2),), -0.2, 0.2)), 0.3, 2.0),
        "output_mean": normal_values(keys[10], (E, R), 0.7, 4.0, ((0, 2),), jnp.float32),
        "output_square": jnp.clip(jnp.exp(math.log(2.0) - 1.89712 * jax.random.uniform(keys[11], (E, R), jnp.float32) ** block_scale(keys[11], (E, R), ((0, 2),), -0.2, 0.2)), 0.3, 2.0),
    }


def reference(block_input, value_cotangent, mixed_output, output_cotangent, value_weight, output_weight, value_basis, output_basis, value_mean, value_square, output_mean, output_square):
    highest = lax.Precision.HIGHEST
    scaling = 1.0 / math.sqrt(TOKENS)
    value_grad = jnp.dot(block_input.T, value_cotangent, preferred_element_type=jnp.float32)
    output_grad = jnp.dot(mixed_output.T, output_cotangent, preferred_element_type=jnp.float32)
    value_base = value_basis.astype(jnp.float32)
    output_base = output_basis.astype(jnp.float32)
    value_low = jnp.dot(value_base.T, value_grad, precision=highest) * scaling
    output_low = jnp.dot(output_grad, output_base, precision=highest) * scaling
    total_squares = jnp.sum(value_low * value_low) + jnp.sum(output_low * output_low)
    clip_scale = 1.0 / jnp.sqrt(1.0 + total_squares / (2.0 * R * E))
    value_scaled = clip_scale * value_low
    output_scaled = clip_scale * output_low
    value_mean_next = 0.8 * value_mean + 0.2 * value_scaled
    output_mean_next = 0.8 * output_mean + 0.2 * output_scaled
    value_square_next = 0.9 * value_square + 0.1 * value_scaled * value_scaled
    output_square_next = 0.9 * output_square + 0.1 * output_scaled * output_scaled
    value_norm = value_mean_next / jnp.sqrt(value_square_next + 0.1)
    output_norm = output_mean_next / jnp.sqrt(output_square_next + 0.1)
    value_step = jnp.dot(value_base, value_norm, precision=highest)
    output_step = jnp.dot(output_norm, output_base.T, precision=highest)
    value_next = value_weight - 0.02 * value_step
    output_next = output_weight - 0.02 * output_step
    return (value_next, value_next.astype(jnp.bfloat16), value_step, value_mean_next, value_square_next, output_next, output_next.astype(jnp.bfloat16), output_step, output_mean_next, output_square_next)
```

```python
import math

import jax
import jax.numpy as jnp
from jax import lax
from jax.sharding import PartitionSpec as P

WEIGHT_SCALE = 2.0**18


def split_wide(wide):
    leading = wide.astype(jnp.bfloat16)
    trailing = (wide - leading.astype(jnp.float32)).astype(jnp.bfloat16)
    return leading, trailing


def split_product(pieces, narrow_right, contract):
    first = lax.dot_general(pieces[0], narrow_right, contract, preferred_element_type=jnp.float32)
    second = lax.dot_general(pieces[1], narrow_right, contract, preferred_element_type=jnp.float32)
    return first + second


def bit_orders(size):
    bits = list(range(size.bit_length() - 1))[::-1]
    return [bits[-r:] + bits[:-r] if r else bits for r in range(3)]


def exchange(value, bit):
    size = lax.axis_size("fs")
    return lax.ppermute(value, "fs", [(i, i ^ (1 << bit)) for i in range(size)])


def my_bit(bit):
    return ((lax.axis_index("fs") >> bit) & 1) == 1


def gather_many(values, orders):
    shapes = [v.shape for v in values]
    held = [[] for _ in values]
    for step in range(len(orders[0])):
        received = [exchange(v, order[step]) for v, order in zip(values, orders)]
        for i, order in enumerate(orders):
            bit = order[step]
            place = sum(1 for b in held[i] if b > bit)
            mine, other, flag = values[i], received[i], my_bit(bit)
            values[i] = jnp.stack([jnp.where(flag, other, mine), jnp.where(flag, mine, other)], axis=place)
            held[i].append(bit)
    return [v.reshape((-1,) + s) for v, s in zip(values, shapes)]


def reduce_scatter_many(values, orders):
    count = len(orders[0])
    values = [v.reshape((2,) * count + v.shape[1:]) for v in values]
    left = [list(range(count))[::-1] for _ in values]
    for step in range(count):
        sends, keeps = [], []
        for i, order in enumerate(orders):
            bit = order[step]
            place = left[i].index(bit)
            low = lax.index_in_dim(values[i], 0, place, keepdims=False)
            high = lax.index_in_dim(values[i], 1, place, keepdims=False)
            flag = my_bit(bit)
            sends.append(jnp.where(flag, low, high))
            keeps.append(jnp.where(flag, high, low))
            left[i].remove(bit)
        received = [exchange(s, order[step]) for s, order in zip(sends, orders)]
        values = [k + r for k, r in zip(keeps, received)]
    return values


def on_device(
    block_input,
    value_cotangent,
    mixed_output,
    output_cotangent,
    value_weight,
    output_weight,
    value_basis,
    output_basis,
    value_mean,
    value_square,
    output_mean,
    output_square,
):
    fs_size = lax.axis_size("fs")
    tp_size = lax.axis_size("tp")
    tokens_all = block_input.shape[0] * fs_size
    scaling = 1.0 / math.sqrt(tokens_all)
    rank_size = value_basis.shape[1]
    local_width = value_cotangent.shape[1]
    contract = (((0,), (0,)), ((), ()))
    orders = bit_orders(fs_size)
    pair = [(t, t ^ 1) for t in range(tp_size)]
    even = lax.axis_index("tp") % 2 == 0

    own_basis = jnp.where(even, value_basis, output_basis)
    gathered = gather_many(jnp.split(own_basis, 3, axis=1), orders)
    swapped = [lax.ppermute(g, "tp", pair) for g in gathered]
    value_full = jnp.concatenate([jnp.where(even, g, s) for g, s in zip(gathered, swapped)], axis=2)
    output_full = jnp.concatenate([jnp.where(even, s, g) for g, s in zip(gathered, swapped)], axis=2)
    value_full = value_full.reshape(-1, rank_size)
    output_full = output_full.reshape(-1, rank_size)

    value_send = (value_weight * WEIGHT_SCALE).astype(jnp.float16)
    output_send = (output_weight * WEIGHT_SCALE).astype(jnp.float16)
    value_send, output_send, value_full, output_full = lax.optimization_barrier(
        (value_send, output_send, value_full, output_full)
    )
    late = orders[0][:-2] + orders[0][-2:][::-1]
    value_blocks, output_blocks = gather_many([value_send, output_send], [orders[0], late])

    input_proj = jnp.dot(block_input, value_full, preferred_element_type=jnp.float32)
    cotangent_proj = jnp.dot(output_cotangent, output_full, preferred_element_type=jnp.float32)
    value_part = split_product(split_wide(input_proj), value_cotangent, contract)
    output_part = split_product(split_wide(cotangent_proj), mixed_output, contract)
    both = jnp.concatenate([value_part, output_part], axis=0) * scaling
    parts = [p.reshape(fs_size, -1, local_width) for p in jnp.split(both, 3, axis=0)]
    summed = reduce_scatter_many(parts, [order[::-1] for order in orders])
    whole = jnp.concatenate([g.reshape(-1, local_width) for g in gather_many(summed, orders)], axis=0)

    total_squares = lax.psum(jnp.sum(whole * whole), "tp")
    value_low = whole[:rank_size]
    output_low = whole[rank_size:].T
    entries = 2.0 * rank_size * local_width * tp_size
    clip_scale = 1.0 / jnp.sqrt(1.0 + total_squares / entries)
    value_scaled = clip_scale * value_low
    output_scaled = clip_scale * output_low
    value_mean_next = 0.8 * value_mean + 0.2 * value_scaled
    output_mean_next = 0.8 * output_mean + 0.2 * output_scaled
    value_square_next = 0.9 * value_square + 0.1 * value_scaled * value_scaled
    output_square_next = 0.9 * output_square + 0.1 * output_scaled * output_scaled
    value_norm = split_wide(value_mean_next / jnp.sqrt(value_square_next + 0.1))
    output_norm = split_wide(output_mean_next / jnp.sqrt(output_square_next + 0.1))
    down = (((1,), (0,)), ((), ()))
    across = (((1,), (1,)), ((), ()))

    def value_product(base):
        return sum(lax.dot_general(base, n, down, preferred_element_type=jnp.float32) for n in value_norm)

    value_step = value_product(value_basis)
    output_step = split_product(output_norm, output_basis, across)
    value_next = value_weight - 0.02 * value_step
    output_next = output_weight - 0.02 * output_step
    value_old = value_blocks.reshape(-1, local_width).astype(jnp.float32) * (1.0 / WEIGHT_SCALE)
    output_old = output_blocks.transpose(1, 0, 2).reshape(local_width, -1).astype(jnp.float32) * (1.0 / WEIGHT_SCALE)
    value_copy = (value_old - 0.02 * value_product(value_full)).astype(jnp.bfloat16)
    output_copy = (output_old - 0.02 * split_product(output_norm, output_full, across)).astype(jnp.bfloat16)
    return (
        value_next,
        value_copy,
        value_step,
        value_mean_next,
        value_square_next,
        output_next,
        output_copy,
        output_step,
        output_mean_next,
        output_square_next,
    )


def solution(mesh):
    placed = (
        P("fs", None),
        P("fs", "tp"),
        P("fs", "tp"),
        P("fs", None),
        P("fs", "tp"),
        P("tp", "fs"),
        P("fs", None),
        P("fs", None),
        P(None, "tp"),
        P(None, "tp"),
        P("tp", None),
        P("tp", None),
    )
    return jax.shard_map(
        on_device,
        mesh=mesh,
        in_specs=placed,
        out_specs=(
            P("fs", "tp"),
            P(None, "tp"),
            P("fs", "tp"),
            P(None, "tp"),
            P(None, "tp"),
            P("tp", "fs"),
            P("tp", None),
            P("tp", "fs"),
            P("tp", None),
            P("tp", None),
        ),
        check_vma=False,
    )
```

```python
import math

import jax
import jax.numpy as jnp
from jax import lax
from jax.sharding import PartitionSpec as P

WEIGHT_SCALE = 2.0**18


def split_wide(wide):
    leading = wide.astype(jnp.bfloat16)
    trailing = (wide - leading.astype(jnp.float32)).astype(jnp.bfloat16)
    return leading, trailing


def rounded_half(weight):
    return lax.reduce_precision(weight * WEIGHT_SCALE, 8, 10).astype(jnp.float16)


def split_product(pieces, narrow_right, contract):
    first = lax.dot_general(pieces[0], narrow_right, contract, preferred_element_type=jnp.float32)
    second = lax.dot_general(pieces[1], narrow_right, contract, preferred_element_type=jnp.float32)
    return first + second


def bit_orders(size):
    bits = list(range(size.bit_length() - 1))[::-1]
    return [bits[-r:] + bits[:-r] if r else bits for r in range(3)]


def exchange(value, bit):
    size = lax.axis_size("fs")
    return lax.ppermute(value, "fs", [(i, i ^ (1 << bit)) for i in range(size)])


def my_bit(bit):
    return ((lax.axis_index("fs") >> bit) & 1) == 1


def gather_step(state, step):
    received = [exchange(value, order[step]) for value, _, order in state]
    result = []
    for (mine, held, order), other in zip(state, received):
        bit = order[step]
        flag = my_bit(bit)
        place = sum(1 for b in held if b > bit)
        joined = jnp.stack([jnp.where(flag, other, mine), jnp.where(flag, mine, other)], axis=place)
        result.append((joined, held + [bit], order))
    return result


def hold(state, others):
    values, others = lax.optimization_barrier(([v for v, _, _ in state], others))
    return [(v, held, order) for v, (_, held, order) in zip(values, state)], others


def gathered_values(state):
    return [v.reshape((-1,) + v.shape[len(held):]) for v, held, _ in state]


def gather_many(values, orders):
    state = [(v, [], order) for v, order in zip(values, orders)]
    for step in range(len(orders[0])):
        state = gather_step(state, step)
    return gathered_values(state)


def reduce_scatter_many(values, orders):
    count = len(orders[0])
    values = [v.reshape((2,) * count + v.shape[1:]) for v in values]
    left = [list(range(count))[::-1] for _ in values]
    for step in range(count):
        sends, keeps = [], []
        for i, order in enumerate(orders):
            bit = order[step]
            place = left[i].index(bit)
            low = lax.index_in_dim(values[i], 0, place, keepdims=False)
            high = lax.index_in_dim(values[i], 1, place, keepdims=False)
            flag = my_bit(bit)
            sends.append(jnp.where(flag, low, high))
            keeps.append(jnp.where(flag, high, low))
            left[i].remove(bit)
        received = [exchange(s, order[step]) for s, order in zip(sends, orders)]
        values = [k + r for k, r in zip(keeps, received)]
    return values


def on_device(
    block_input,
    value_cotangent,
    mixed_output,
    output_cotangent,
    value_weight,
    output_weight,
    value_basis,
    output_basis,
    value_mean,
    value_square,
    output_mean,
    output_square,
):
    fs_size = lax.axis_size("fs")
    tp_size = lax.axis_size("tp")
    tokens_all = block_input.shape[0] * fs_size
    scaling = 1.0 / math.sqrt(tokens_all)
    rank_size = value_basis.shape[1]
    local_width = value_cotangent.shape[1]
    contract = (((0,), (0,)), ((), ()))
    orders = bit_orders(fs_size)
    pair = [(t, t ^ 1) for t in range(tp_size)]
    even = lax.axis_index("tp") % 2 == 0

    steps = len(orders[0])
    own_basis = jnp.where(even, value_basis, output_basis)
    bases = [(v, [], order) for v, order in zip(jnp.split(own_basis, 3, axis=1), orders)]
    for step in range(steps - 1):
        bases = gather_step(bases, step)
    bases, (value_held, output_held, output_mean, output_square) = hold(
        bases, (value_weight, output_weight, output_mean, output_square)
    )
    late = orders[0][:-2] + orders[0][-2:][::-1]
    weights = [(rounded_half(value_held), [], orders[0]), (rounded_half(output_held), [], late)]
    bases = gather_step(bases, steps - 1)
    for step in range(steps - 2):
        weights = gather_step(weights, step)
    gathered = gathered_values(bases)
    swapped = [lax.ppermute(g, "tp", pair) for g in gathered]
    value_full = jnp.concatenate([jnp.where(even, g, s) for g, s in zip(gathered, swapped)], axis=2)
    output_full = jnp.concatenate([jnp.where(even, s, g) for g, s in zip(gathered, swapped)], axis=2)
    value_full = value_full.reshape(-1, rank_size)
    output_full = output_full.reshape(-1, rank_size)

    weights, (value_full, output_full) = hold(weights, (value_full, output_full))
    weights = gather_step(weights, steps - 2)
    input_proj = jnp.dot(block_input, value_full, preferred_element_type=jnp.float32)
    cotangent_proj = jnp.dot(output_cotangent, output_full, preferred_element_type=jnp.float32)
    value_part = split_product(split_wide(input_proj), value_cotangent, contract)
    output_part = split_product(split_wide(cotangent_proj), mixed_output, contract)
    both = jnp.concatenate([value_part, output_part], axis=0) * scaling
    parts = [p.reshape(fs_size, -1, local_width) for p in jnp.split(both, 3, axis=0)]
    summed = reduce_scatter_many(parts, [order[::-1] for order in orders])
    weights, summed = hold(weights, summed)
    value_blocks, output_blocks = gathered_values(gather_step(weights, steps - 1))
    whole = jnp.concatenate([g.reshape(-1, local_width) for g in gather_many(summed, orders)], axis=0)

    total_squares = lax.psum(jnp.sum(whole * whole), "tp")
    value_low = whole[:rank_size]
    output_low = whole[rank_size:].T
    entries = 2.0 * rank_size * local_width * tp_size
    clip_scale = 1.0 / jnp.sqrt(1.0 + total_squares / entries)
    value_scaled = clip_scale * value_low
    output_scaled = clip_scale * output_low
    value_mean_next = 0.8 * value_mean + 0.2 * value_scaled
    output_mean_next = 0.8 * output_mean + 0.2 * output_scaled
    value_square_next = 0.9 * value_square + 0.1 * value_scaled * value_scaled
    output_square_next = 0.9 * output_square + 0.1 * output_scaled * output_scaled
    value_norm = split_wide(value_mean_next / jnp.sqrt(value_square_next + 0.1))
    output_norm = split_wide(output_mean_next / jnp.sqrt(output_square_next + 0.1))
    down = (((1,), (0,)), ((), ()))
    across = (((1,), (1,)), ((), ()))

    def value_product(base):
        return sum(lax.dot_general(base, n, down, preferred_element_type=jnp.float32) for n in value_norm)

    value_step = value_product(value_basis)
    output_step = split_product(output_norm, output_basis, across)
    value_next = value_weight - 0.02 * value_step
    output_next = output_weight - 0.02 * output_step
    value_old = value_blocks.reshape(-1, local_width).astype(jnp.float32) * (1.0 / WEIGHT_SCALE)
    output_old = output_blocks.transpose(1, 0, 2).reshape(local_width, -1).astype(jnp.float32) * (1.0 / WEIGHT_SCALE)
    value_copy = (value_old - 0.02 * value_product(value_full)).astype(jnp.bfloat16)
    output_copy = (output_old - 0.02 * split_product(output_norm, output_full, across)).astype(jnp.bfloat16)
    return (
        value_next,
        value_copy,
        value_step,
        value_mean_next,
        value_square_next,
        output_next,
        output_copy,
        output_step,
        output_mean_next,
        output_square_next,
    )


def solution(mesh):
    placed = (
        P("fs", None),
        P("fs", "tp"),
        P("fs", "tp"),
        P("fs", None),
        P("fs", "tp"),
        P("tp", "fs"),
        P("fs", None),
        P("fs", None),
        P(None, "tp"),
        P(None, "tp"),
        P("tp", None),
        P("tp", None),
    )
    return jax.shard_map(
        on_device,
        mesh=mesh,
        in_specs=placed,
        out_specs=(
            P("fs", "tp"),
            P(None, "tp"),
            P("fs", "tp"),
            P(None, "tp"),
            P(None, "tp"),
            P("tp", "fs"),
            P("tp", None),
            P("tp", "fs"),
            P("tp", None),
            P("tp", None),
        ),
        check_vma=False,
    )
```
